512 devices in a mesh: sp: 32 (over z, x), dp: 16 (over y, core).
Axes of the slice: x: 4, y: 8, z: 8, core: 2. Of those that a mesh axis runs over, the one named last changes fastest.
Arguments:
- tokens: bfloat16 [16, 16384, 2048], P('dp', 'sp'), may hold values from -6 to 6
- segments: int32 [16, 16384], P('dp', 'sp'), may hold values from 0 to 15, never falling along the last dimension, each value on 1 to 2048 neighbouring positions
- w_lin: bfloat16 [2048, 1024], P('dp'), may hold values from -0.125 to 0.125
- w_gate: bfloat16 [2048, 1024], P('dp'), may hold values from -0.125 to 0.125
- w_out: bfloat16 [1024, 2048], P(None, 'dp'), may hold values from -0.1875 to 0.1875
- conv_kernel: float32 [31, 1024], replicated, may hold values from -1 to 1
- conv_bias: float32 [1024], replicated, may hold values from -3 to 3
- norm_gain: float32 [1024], replicated, may hold values from 0.1 to 1.9
- norm_bias: float32 [1024], replicated, may hold values from -3 to 3
Outputs:
- mixed_out: bfloat16 [16, 16384, 2048], P('dp', 'sp')
The draws below stay inside these ranges and needn't reach their ends.
Inputs may be any that keep to these rules, and one draw needn't show every extreme that they name: `segments`: within each sequence document numbers never fall; a document is a run of equal numbers of at most four times 512 positions.
All inputs are finite; a program needn't handle non-finite values.
Results may differ from the reference program's by a relative error of at most 0.0062.
Values may be sent and summed in bfloat16 or wider, within the bound.
A program may use at most 64 MiB of HBM per device.

```python
import math
import jax
import jax.numpy as jnp
import numpy as np
from jax import lax

D = 2048
CW = 1024
K = 31
TOK_DEV = 512
SEQ = 16384
SEQS = 16
N_SP = 32


def steps_of(stream_key, shape, cuts, least, high):
    factor_of, own = 1.0, jax.random.fold_in(stream_key, 6)
    for axis_at, parts in cuts:
        heights = jnp.exp(jax.random.uniform(jax.random.fold_in(own, axis_at), (parts,), jnp.float32, least / len(cuts), high / len(cuts)))
        factor_of = factor_of * jnp.repeat(heights, shape[axis_at] // parts).reshape([-1 if axis == axis_at else 1 for axis in range(len(shape))])
    return factor_of


def length_profile(number_of, total, reach, slope):
    weights = [(1 << 20) // math.isqrt(grade ** slope) + 1 for grade in range(2, number_of + 1)]
    spare, holding = total - reach - (number_of - 1), [1] * (number_of - 1)
    while spare > 0:
        candidates = [i for i in range(number_of - 1) if holding[i] < reach]
        whole, remaining = sum([weights[i] for i in candidates]), spare
        for i in candidates:
            extra = min(reach - holding[i], max(1, remaining * weights[i] // whole), spare)
            holding[i] = holding[i] + extra
            spare = spare - extra
    return np.array([reach] + holding)


def uneven_parts(own_key, count, total, bound, lean):
    if count == 2:
        one = jax.random.randint(own_key, (), max(1, total - bound), min(bound, total - 1) + 1)
        return jnp.stack([one, total - one])
    sizes = jnp.asarray(length_profile(count, total, bound, lean), jnp.int32)
    couples = (count - 1) // 2
    source_of, receiver = sizes[1:1 + 2 * couples:2], sizes[2:2 + 2 * couples:2]
    room = jnp.minimum(source_of - 1, bound - receiver)
    moved = jax.random.randint(jax.random.fold_in(own_key, 1), (couples,), 0, 1 << 20) % (room + 1)
    sizes = sizes.at[1:1 + 2 * couples:2].set(source_of - moved).at[2:2 + 2 * couples:2].set(receiver + moved)
    return sizes[jax.random.permutation(jax.random.fold_in(own_key, 2), count)]


def normal_values(rng, dims, width, limit, cuts=(), held_as=jnp.bfloat16):
    drawn = width * jax.random.normal(rng, dims, jnp.float32)
    if cuts:
        drawn = drawn * steps_of(rng, dims, cuts, -0.22, 0.18)
    return jnp.clip(drawn, -limit, limit).astype(held_as)


def setup_inputs(seed: int = 0) -> dict:
    streams_of = jax.random.split(jax.random.key(seed), 10)
    return {
        "tokens": normal_values(streams_of[0], (SEQS, SEQ, D), 1.0, 6.0, ((0, 16), (1, 32))),
        "segments": jax.vmap(lambda own: jnp.searchsorted(jnp.cumsum(uneven_parts(own, N_SP // 2, SEQ, 4 * TOK_DEV, 2)), jnp.arange(SEQ), side="right"))(jax.random.split(streams_of[1], SEQS)).reshape((SEQS, SEQ)).astype(jnp.int32),
        "w_lin": normal_values(streams_of[2], (D, CW), D ** -0.5, 0.125, ((0, 16),)),
        "w_gate": normal_values(streams_of[3], (D, CW), D ** -0.5, 0.125, ((0, 16),)),
        "w_out": normal_values(streams_of[4], (CW, D), CW ** -0.5, 0.1875, ((1, 16),)),
        "conv_kernel": normal_values(streams_of[5], (K, CW), K ** -0.5, 1.0, (), jnp.float32),
        "conv_bias": normal_values(streams_of[6], (CW,), 0.5, 3.0, (), jnp.float32),
        "norm_gain": jnp.clip(1.0 + 0.18 * jax.random.normal(streams_of[7], (CW,), jnp.float32), 0.1, 1.9),
        "norm_bias": normal_values(streams_of[8], (CW,), 0.5, 3.0, (), jnp.float32),
    }


def conv_doc(values, doc_ids, kernel, bias):
    length = values.shape[1]
    taps = kernel.shape[0]
    total = bias[:, None] + kernel[taps - 1][:, None] * values
    for back in range(1, taps):
        shifted = jnp.pad(values[:, :length - back], ((0, 0), (back, 0)))
        same = jnp.pad(doc_ids[back:] == doc_ids[:length - back], (back, 0))
        total = total + kernel[taps - 1 - back][:, None] * jnp.where(same[None, :], shifted, 0.0)
    return total

def reference(tokens, segments, w_lin, w_gate, w_out, conv_kernel, conv_bias, norm_gain, norm_bias):

    def one_sequence(pair):
        rows, doc_ids = pair
        lin = jnp.dot(rows, w_lin, preferred_element_type=jnp.float32)
        gate = jnp.dot(rows, w_gate, preferred_element_type=jnp.float32)
        glu = (lin * jax.nn.sigmoid(gate)).astype(jnp.bfloat16)
        conv = conv_doc(glu.T.astype(jnp.float32), doc_ids, conv_kernel, conv_bias)
        values = lax.optimization_barrier(conv.astype(jnp.bfloat16)).astype(jnp.float32)
        mean = lax.optimization_barrier(jnp.mean(values, axis=0, keepdims=True))
        var = lax.optimization_barrier(jnp.mean(jnp.square(values - mean), axis=0, keepdims=True))
        normed = (values - mean) * lax.rsqrt(var + 1e-05) * norm_gain[:, None] + norm_bias[:, None]
        act = jax.nn.silu(normed).astype(jnp.bfloat16)
        return jnp.dot(act.T, w_out, preferred_element_type=jnp.float32).astype(jnp.bfloat16)
    return lax.map(one_sequence, (tokens, segments))
```

```python
import functools

import jax
import jax.numpy as jnp
from jax import lax
from jax.experimental import pallas as pl
from jax.experimental.pallas import tpu as pltpu
from jax.sharding import PartitionSpec as P

MESH = pl.DeviceIdType.MESH
F32, BF16 = jnp.float32, jnp.bfloat16
NX, NY, NZ = 4, 8, 8
UNITS, IN_UNITS = 12, 8
TOK, TAIL, ROWS = 512, 32, 544
TAPS = 31
LEAD_SEND, LEAD_FORWARD, LEAD_FAR, LEAD_NEAR_PAIR, LEAD_FAR_PAIR = 5, 3, 2, 2, 1


def offset_of(e):
    return ((e + 1) // 2) * (2 * (e % 2) - 1)


def kernel(
    tok, seg, wl, wg, wo, ck, cb, ng, nb, out,
    w, x, ids, idc, dist, taps, ckv, vecs, g, conv, act, ost,
    load_sem, misc_sem, recv_sem, send_sem,
):
    sp, dp = lax.axis_index("sp"), lax.axis_index("dp")
    px, pz = sp % NX, sp // NX
    py, pc = dp // 2, dp % 2

    def at(dx=0, dy=0, dz=0):
        return (
            ((pz + dz + NZ) % NZ) * NX + (px + dx + NX) % NX,
            ((py + dy + NY) % NY) * 2 + pc,
        )

    after = ((sp + 1) % (NX * NZ), dp)
    before = ((sp + NX * NZ - 1) % (NX * NZ), dp)
    partner = (sp, py * 2 + 1 - pc)

    def local(src, dst, sem):
        pltpu.make_async_copy(src, dst, sem).start()

    def wait(region, sem):
        pltpu.make_async_copy(region, region, sem).wait()

    for u in range(IN_UNITS):
        lanes = pl.ds(128 * u, 128)
        local(wl.at[:, :, lanes], w.at[u, 0, pc, :, :, pl.ds(0, 128)], load_sem.at[u])
        local(wg.at[:, :, lanes], w.at[u, 0, pc, :, :, pl.ds(128, 128)], load_sem.at[u])
    for e in range(8):
        src = pl.multiple_of(256 * ((py + offset_of(e) + NY) % NY), 256)
        local(tok.at[:, pl.ds(src, 256)], x.at[pl.ds(TAIL, TOK), pl.ds(256 * e, 256)], misc_sem.at[0])
    local(seg, ids.at[:, pl.ds(128, TOK)], misc_sem.at[1])
    for u in range(8):
        local(wo.at[u], w.at[8 + u // 2, 0, pc, :, :, pl.ds(128 * (u % 2), 128)], load_sem.at[8 + u // 2])
    local(ck, ckv, misc_sem.at[2])
    local(cb, vecs.at[0], misc_sem.at[3])
    local(ng, vecs.at[1], misc_sem.at[4])
    local(nb, vecs.at[2], misc_sem.at[5])

    barrier = pltpu.get_barrier_semaphore()
    peers = [at(dy=1), at(dy=-1), at(dy=2), at(dy=-2), at(dx=1), at(dx=-1), at(dz=1), at(dz=-1),
             partner, after, before]
    for peer in peers:
        pl.semaphore_signal(barrier, inc=1, device_id=peer, device_id_type=MESH)
    pl.semaphore_wait(barrier, len(peers))

    def send(ref, kind, unit, peer, dst=None):
        pltpu.make_async_remote_copy(
            src_ref=ref, dst_ref=ref if dst is None else dst,
            send_sem=send_sem.at[kind], recv_sem=recv_sem.at[kind, unit],
            device_id=peer, device_id_type=MESH,
        ).start()

    def class_of(parity):
        return (px * (1 + parity) + pz * (2 - parity)) % 4

    def planes(parity):
        def mix(a, b):
            return tuple((1 - parity) * i + parity * j for i, j in zip(a, b))
        return (mix(at(dx=1), at(dz=1)), mix(at(dx=-1), at(dz=-1)),
                mix(at(dz=1), at(dx=1)), mix(at(dz=-1), at(dx=-1)))

    def in_plane(m, first, count, kind):
        parity = m % 2
        q = class_of(parity)
        heavy_up, heavy_down, light_up, light_down = planes(parity)
        span = pl.ds(first, count)
        whole = w.at[m, span, pc, q]
        send(whole, kind, m, heavy_up)
        send(whole, kind, m, heavy_down)
        send(w.at[m, span, pc, q, pl.ds(0, 16), :], kind, m, light_up)
        send(w.at[m, span, pc, q, pl.ds(16, 16), :], kind, m, light_down)

    def prepare():
        wait(seg, misc_sem.at[1])
        wait(x.at[pl.ds(TAIL, TOK), :], misc_sem.at[0])
        pltpu.make_async_remote_copy(
            src_ref=x.at[pl.ds(TOK, TAIL), :], dst_ref=x.at[pl.ds(0, TAIL), :],
            send_sem=misc_sem.at[6], recv_sem=misc_sem.at[7],
            device_id=after, device_id_type=MESH,
        ).start()
        pltpu.make_async_remote_copy(
            src_ref=ids.at[:, pl.ds(TOK, 128)], dst_ref=ids.at[:, pl.ds(0, 128)],
            send_sem=misc_sem.at[8], recv_sem=misc_sem.at[9],
            device_id=after, device_id_type=MESH,
        ).start()

    def masks():
        wait(ck, misc_sem.at[2])
        wait(cb, misc_sem.at[3])
        wait(ng, misc_sem.at[4])
        wait(nb, misc_sem.at[5])

        def spread(u, _):
            lanes = pl.ds(pl.multiple_of(128 * u, 128), 128)
            for k in range(TAPS):
                taps[u, k] = jnp.broadcast_to(ckv[pl.ds(TAPS - 1 - k, 1), lanes], (8, 128))
            taps[u, TAPS] = jnp.broadcast_to(vecs[0, pl.ds(u, 1), :], (8, 128))
            return 0

        lax.fori_loop(0, 8, spread, 0)
        g[pl.ds(0, 8), :] = jnp.zeros((8, 128), F32)
        wait(ids.at[:, pl.ds(0, 128)], misc_sem.at[9])
        wait(x.at[pl.ds(0, TAIL), :], misc_sem.at[7])
        for b in range(5):
            row = ids[:, pl.ds(128 * b, 128)]
            if b == 0:
                row = jnp.where(sp == 0, -1, row)
            idc[pl.ds(128 * b, 128), :] = jnp.broadcast_to(row, (128, 128)).T

        def count(i, _):
            base = pl.multiple_of(8 * i, 8)
            here = idc[pl.ds(base + 96, 8), :]
            total = jnp.zeros((8, 128), jnp.int32)
            for k in range(1, TAPS):
                total = total + jnp.where(idc[pl.ds(base + 96 - k, 8), :] == here, 1, 0)
            dist[pl.ds(base, 8), :] = total
            return 0

        lax.fori_loop(0, ROWS // 8, count, 0)

    def compute(u):
        wu = w[u].reshape(2048, 256)
        half = ROWS // 2
        for i in range(2):
            r = jnp.dot(x[pl.ds(half * i, half), :], wu, preferred_element_type=F32)
            glu = r[:, :128] * jax.nn.sigmoid(r[:, 128:])
            g[pl.ds(8 + half * i, half), :] = glu.astype(BF16).astype(F32)

        def parts(i, wanted):
            base = pl.multiple_of(8 * i, 8)
            d = dist[pl.ds(base, 8), :]
            m = [g[pl.ds(base + 8, 8), :]]
            for j in range(1, 8):
                m.append(jnp.where(d >= j, g[pl.ds(base + 8 - j, 8), :], 0.0))
            sums = []
            for j in range(4):
                total = None
                if j in wanted:
                    for i8 in range(8):
                        if 8 * j + i8 < TAPS:
                            term = taps[u, 8 * j + i8] * m[i8]
                            total = term if total is None else total + term
                sums.append(total)
            return d, sums

        def step(i, carry):
            p1, p2, p3, q2, q3, r3 = carry
            results = []
            for s in range(4):
                d, (s0, s1, s2, s3) = parts(4 * i + s, (0, 1, 2, 3))
                total = taps[u, TAPS] + s0 + jnp.where(d >= 8, p1, 0.0)
                total = total + jnp.where(d >= 16, q2, 0.0) + jnp.where(d >= 24, r3, 0.0)
                results.append(total)
                p1, p2, p3, q2, q3, r3 = s1, s2, s3, p2, p3, q3
            base = pl.multiple_of(32 * i - TAIL, 32)
            conv[u, pl.ds(base, 32), :] = jnp.concatenate(results, axis=0).astype(BF16).astype(F32)
            return p1, p2, p3, q2, q3, r3

        _, (_, _, _, r3) = parts(1, (3,))
        _, (_, _, q2, q3) = parts(2, (2, 3))
        _, (_, p1, p2, p3) = parts(3, (1, 2, 3))
        lax.fori_loop(1, ROWS // 32, step, (p1, p2, p3, q2, q3, r3))

    def normalize():
        def step(i, _):
            rows = pl.ds(pl.multiple_of(64 * i, 64), 64)
            total = conv[0, rows, :]
            for u in range(1, 8):
                total = total + conv[u, rows, :]
            mean = jnp.sum(total, axis=1, keepdims=True) * (1.0 / 1024)
            square = None
            for u in range(8):
                off = conv[u, rows, :] - mean
                square = off * off if square is None else square + off * off
            var = jnp.sum(square, axis=1, keepdims=True) * (1.0 / 1024)
            scale = lax.rsqrt(var + 1e-05)
            for u in range(8):
                v = (conv[u, rows, :] - mean) * scale * vecs[1, pl.ds(u, 1), :] + vecs[2, pl.ds(u, 1), :]
                act[rows, pl.ds(128 * u, 128)] = (v * jax.nn.sigmoid(v)).astype(BF16)
            return 0

        lax.fori_loop(0, TOK // 64, step, 0)

    def slot(s, _):
        def stage(lead):
            m = s + lead
            return m, jnp.logical_and(m >= 0, m < UNITS)

        m0, on0 = stage(LEAD_SEND)

        @pl.when(on0)
        def _():
            wait(w.at[m0, 0, pc], load_sem.at[m0])
            own = w.at[m0, 0, pc, class_of(m0 % 2)]
            q = class_of(m0 % 2)
            for e, dy in ((2, 1), (1, -1), (4, 2), (3, -2)):
                send(own, 0, m0, at(dy=dy), w.at[m0, e, pc, q])
            send(w.at[m0, 0, pc], 4, m0, partner)

        @pl.when(s == 1 - LEAD_SEND)
        def _():
            prepare()

        m1, on1 = stage(LEAD_FORWARD)

        @pl.when(on1)
        def _():
            q = class_of(m1 % 2)
            wait(w.at[m1, pl.ds(1, 4), pc, q], recv_sem.at[0, m1])
            send(w.at[m1, 4, pc, q], 1, m1, at(dy=1), w.at[m1, 6, pc, q])
            send(w.at[m1, 3, pc, q], 1, m1, at(dy=-1), w.at[m1, 5, pc, q])
            low, high = pl.ds(0, 16), pl.ds(16, 16)
            send(w.at[m1, 4, pc, q, low, :], 1, m1, at(dy=2), w.at[m1, 7, pc, q, low, :])
            send(w.at[m1, 3, pc, q, high, :], 1, m1, at(dy=-2), w.at[m1, 7, pc, q, high, :])
            in_plane(m1, 1, 4, 2)

        m2, on2 = stage(LEAD_FAR)

        @pl.when(on2)
        def _():
            wait(w.at[m2, pl.ds(5, 3), pc, class_of(m2 % 2)], recv_sem.at[1, m2])
            in_plane(m2, 5, 3, 3)

        m3, on3 = stage(LEAD_NEAR_PAIR)

        @pl.when(on3)
        def _():
            wait(w.at[m3, pl.ds(1, 3), pc], recv_sem.at[2, m3])
            send(w.at[m3, pl.ds(1, 4), pc], 4, m3, partner)

        m4, on4 = stage(LEAD_FAR_PAIR)

        @pl.when(on4)
        def _():
            wait(w.at[m4, pl.ds(1, 3), pc, pl.ds(0, 3)], recv_sem.at[3, m4])
            send(w.at[m4, pl.ds(5, 3), pc], 4, m4, partner)

        @pl.when(s == -1)
        def _():
            masks()

        @pl.when(s >= 0)
        def _():
            wait(w.at[s, :, 1 - pc], recv_sem.at[4, s])

        @pl.when(jnp.logical_and(s >= 0, s < IN_UNITS))
        def _():
            compute(s)

        @pl.when(s == IN_UNITS - 1)
        def _():
            normalize()

        return 0

    lax.fori_loop(-LEAD_SEND, UNITS, slot, 0)

    def project(e, _):
        blocks = []
        for v in range(4):
            for h in range(2):
                lanes = pl.ds(128 * h, 128)
                blocks.append(jnp.concatenate(
                    [w[IN_UNITS + v, e, c, :, :, lanes].reshape(128, 128) for c in range(2)], axis=1))
        rhs = jnp.concatenate(blocks, axis=0)
        ost[e] = jnp.dot(act[...], rhs, preferred_element_type=F32).astype(BF16)
        dst = pl.multiple_of(256 * ((py + offset_of(e) + NY) % NY), 256)
        pltpu.make_async_copy(ost.at[e], out.at[:, pl.ds(dst, 256)], misc_sem.at[10]).start()
        return 0

    lax.fori_loop(0, 8, project, 0)

    wait(w.at[:, pl.ds(1, 4), 0, 0], send_sem.at[0])
    wait(w.at[:, pl.ds(5, 3), 0, 0], send_sem.at[1])
    wait(w.at[:, pl.ds(1, 3), 0], send_sem.at[2])
    wait(w.at[:, pl.ds(1, 3), 0, pl.ds(0, 3)], send_sem.at[3])
    wait(w.at[:, :, 0], send_sem.at[4])
    wait(x.at[pl.ds(0, TAIL), :], misc_sem.at[6])
    wait(ids.at[:, pl.ds(0, 128)], misc_sem.at[8])
    wait(ost, misc_sem.at[10])


def body(tokens, segments, w_lin, w_gate, w_out, conv_kernel, conv_bias, norm_gain, norm_bias):
    anywhere = pl.BlockSpec(memory_space=pl.ANY)
    result = pl.pallas_call(
        kernel,
        out_shape=jax.ShapeDtypeStruct((TOK, 2048), BF16),
        in_specs=[anywhere] * 9,
        out_specs=anywhere,
        scratch_shapes=[
            pltpu.VMEM((UNITS, 8, 2, 4, 32, 256), BF16),
            pltpu.VMEM((ROWS, 2048), BF16),
            pltpu.VMEM((1, 128 + TOK), jnp.int32),
            pltpu.VMEM((128 + TOK, 128), jnp.int32),
            pltpu.VMEM((ROWS, 128), jnp.int32),
            pltpu.VMEM((8, 32, 8, 128), F32),
            pltpu.VMEM((TAPS, 1024), F32),
            pltpu.VMEM((3, 8, 128), F32),
            pltpu.VMEM((8 + ROWS, 128), F32),
            pltpu.VMEM((8, TOK, 128), F32),
            pltpu.VMEM((TOK, 1024), BF16),
            pltpu.VMEM((8, TOK, 256), BF16),
            pltpu.SemaphoreType.DMA((UNITS,)),
            pltpu.SemaphoreType.DMA((11,)),
            pltpu.SemaphoreType.DMA((5, UNITS)),
            pltpu.SemaphoreType.DMA((5,)),
        ],
        compiler_params=pltpu.CompilerParams(
            collective_id=0, has_side_effects=True, vmem_limit_bytes=48 * 1024 * 1024
        ),
    )(
        tokens[0],
        segments,
        w_lin.reshape(4, 32, 1024),
        w_gate.reshape(4, 32, 1024),
        w_out.reshape(8, 4, 32, 128),
        conv_kernel,
        conv_bias.reshape(8, 128),
        norm_gain.reshape(8, 128),
        norm_bias.reshape(8, 128),
    )
    return result[None]


def solution(mesh):
    placed = (
        P("dp", "sp", None),
        P("dp", "sp"),
        P("dp", None),
        P("dp", None),
        P(None, "dp"),
        P(),
        P(),
        P(),
        P(),
    )
    return jax.shard_map(
        body, mesh=mesh, in_specs=placed, out_specs=P("dp", "sp", None), check_vma=False
    )
```

```python
import functools

import jax
import jax.numpy as jnp
from jax import lax
from jax.experimental import pallas as pl
from jax.experimental.pallas import tpu as pltpu
from jax.sharding import PartitionSpec as P

MESH = pl.DeviceIdType.MESH
F32, BF16 = jnp.float32, jnp.bfloat16
NX, NY, NZ = 4, 8, 8
UNITS, IN_UNITS = 12, 8
TOK, TAIL, ROWS = 512, 32, 544
TAPS = 31
LEAD_SEND, LEAD_FORWARD, LEAD_FAR, LEAD_NEAR_PAIR, LEAD_FAR_PAIR = 11, 8, 5, 5, 2


def offset_of(e):
    return ((e + 1) // 2) * (2 * (e % 2) - 1)


def kernel(
    tok, seg, wl, wg, wo, ck, cb, ng, nb, out,
    w, x, ids, idc, dist, taps, ckv, vecs, g, conv, act,
    load_sem, misc_sem, recv_sem, send_sem,
):
    sp, dp = lax.axis_index("sp"), lax.axis_index("dp")
    px, pz = sp % NX, sp // NX
    py, pc = dp // 2, dp % 2

    def at(dx=0, dy=0, dz=0):
        return (
            ((pz + dz + NZ) % NZ) * NX + (px + dx + NX) % NX,
            ((py + dy + NY) % NY) * 2 + pc,
        )

    after = ((sp + 1) % (NX * NZ), dp)
    before = ((sp + NX * NZ - 1) % (NX * NZ), dp)
    partner = (sp, py * 2 + 1 - pc)

    def local(src, dst, sem):
        pltpu.make_async_copy(src, dst, sem).start()

    def wait(region, sem):
        pltpu.make_async_copy(region, region, sem).wait()

    for u in range(IN_UNITS):
        lanes = pl.ds(128 * u, 128)
        local(wl.at[:, :, lanes], w.at[u, 0, pc, :, :, pl.ds(0, 128)], load_sem.at[u])
        local(wg.at[:, :, lanes], w.at[u, 0, pc, :, :, pl.ds(128, 128)], load_sem.at[u])
    for e in range(8):
        src = pl.multiple_of(256 * ((py + offset_of(e) + NY) % NY), 256)
        local(tok.at[:, pl.ds(src, 256)], x.at[pl.ds(TAIL, TOK), pl.ds(256 * e, 256)], misc_sem.at[0])
    local(seg, ids.at[:, pl.ds(128, TOK)], misc_sem.at[1])
    for u in range(8):
        local(wo.at[u], w.at[8 + u // 2, 0, pc, :, :, pl.ds(128 * (u % 2), 128)], load_sem.at[8 + u // 2])
    local(ck, ckv, misc_sem.at[2])
    local(cb, vecs.at[0], misc_sem.at[3])
    local(ng, vecs.at[1], misc_sem.at[4])
    local(nb, vecs.at[2], misc_sem.at[5])

    barrier = pltpu.get_barrier_semaphore()
    peers = [at(dy=1), at(dy=-1), at(dy=2), at(dy=-2), at(dx=1), at(dx=-1), at(dz=1), at(dz=-1),
             partner, after, before]
    for peer in peers:
        pl.semaphore_signal(barrier, inc=1, device_id=peer, device_id_type=MESH)
    pl.semaphore_wait(barrier, len(peers))

    def send(ref, kind, unit, peer, dst=None):
        pltpu.make_async_remote_copy(
            src_ref=ref, dst_ref=ref if dst is None else dst,
            send_sem=send_sem.at[kind], recv_sem=recv_sem.at[kind, unit],
            device_id=peer, device_id_type=MESH,
        ).start()

    def kind_of(m):
        return 1 - (((m + 1) * 5) // UNITS - (m * 5) // UNITS)

    for e in range(8):
        src = pl.multiple_of(256 * ((py + offset_of(e) + NY) % NY), 256)
        pltpu.make_async_remote_copy(
            src_ref=tok.at[pl.ds(TOK - TAIL, TAIL), pl.ds(src, 256)],
            dst_ref=x.at[pl.ds(0, TAIL), pl.ds(256 * e, 256)],
            send_sem=misc_sem.at[6], recv_sem=misc_sem.at[7],
            device_id=after, device_id_type=MESH,
        ).start()
    pltpu.make_async_remote_copy(
        src_ref=seg.at[:, pl.ds(TOK - 128, 128)], dst_ref=ids.at[:, pl.ds(0, 128)],
        send_sem=misc_sem.at[8], recv_sem=misc_sem.at[9],
        device_id=after, device_id_type=MESH,
    ).start()

    def class_of(parity):
        return (px * (1 + parity) + pz * (2 - parity)) % 4

    def planes(parity):
        def mix(a, b):
            return tuple((1 - parity) * i + parity * j for i, j in zip(a, b))
        return (mix(at(dx=1), at(dz=1)), mix(at(dx=-1), at(dz=-1)),
                mix(at(dz=1), at(dx=1)), mix(at(dz=-1), at(dx=-1)))

    def in_plane(m, first, count, kind):
        parity = kind_of(m)
        q = class_of(parity)
        heavy_up, heavy_down, light_up, light_down = planes(parity)
        span = pl.ds(first, count)
        whole = w.at[m, span, pc, q]
        send(whole, kind, m, heavy_up)
        send(whole, kind, m, heavy_down)
        send(w.at[m, span, pc, q, pl.ds(0, 16), :], kind, m, light_up)
        send(w.at[m, span, pc, q, pl.ds(16, 16), :], kind, m, light_down)

    def spread_taps():
        wait(ck, misc_sem.at[2])
        wait(cb, misc_sem.at[3])
        wait(ng, misc_sem.at[4])
        wait(nb, misc_sem.at[5])

        def spread(u, _):
            lanes = pl.ds(pl.multiple_of(128 * u, 128), 128)
            for k in range(TAPS):
                taps[u, k] = jnp.broadcast_to(ckv[pl.ds(TAPS - 1 - k, 1), lanes], (8, 128))
            taps[u, TAPS] = jnp.broadcast_to(vecs[0, pl.ds(u, 1), :], (8, 128))
            return 0

        lax.fori_loop(0, 8, spread, 0)
        g[pl.ds(0, 8), :] = jnp.zeros((8, 128), F32)

    def masks():
        wait(seg, misc_sem.at[1])
        wait(ids.at[:, pl.ds(0, 128)], misc_sem.at[9])
        for b in range(5):
            row = ids[:, pl.ds(128 * b, 128)]
            if b == 0:
                row = jnp.where(sp == 0, -1, row)
            idc[pl.ds(128 * b, 128), :] = jnp.broadcast_to(row, (128, 128)).T

        def count(i, _):
            base = pl.multiple_of(8 * i, 8)
            here = idc[pl.ds(base + 96, 8), :]
            total = jnp.zeros((8, 128), jnp.int32)
            for k, more in ((1, 1), (2, 1), (3, 1), (4, 1), (5, 1), (6, 1), (7, 1), (8, 1), (16, 8), (24, 8)):
                total = total + jnp.where(idc[pl.ds(base + 96 - k, 8), :] == here, more, 0)
            dist[pl.ds(base, 8), :] = total
            return 0

        lax.fori_loop(0, ROWS // 8, count, 0)

    def compute(u):
        wu = w[u].reshape(2048, 256)
        half = ROWS // 2
        for i in range(2):
            r = jnp.dot(x[pl.ds(half * i, half), :], wu, preferred_element_type=F32)
            lin = 0.5 * r[:, :128]
            glu = lin + lin * jnp.tanh(0.5 * r[:, 128:])
            g[pl.ds(8 + half * i, half), :] = glu.astype(BF16).astype(F32)

        def shifted(i):
            base = pl.multiple_of(8 * i, 8)
            d = dist[pl.ds(base, 8), :]
            m = [g[pl.ds(base + 8, 8), :]]
            for j in range(1, 8):
                m.append(jnp.where(d >= j, g[pl.ds(base + 8 - j, 8), :], 0.0))
            return d, m

        def sums(j, ms):
            totals = [None] * len(ms)
            for i8 in range(8):
                if 8 * j + i8 < TAPS:
                    tap = taps[u, 8 * j + i8]
                    for n, m in enumerate(ms):
                        term = tap * m[i8]
                        totals[n] = term if totals[n] is None else totals[n] + term
            return totals

        def step(i, carry):
            p1, p2, p3, q2, q3, r3 = carry
            ds, ms = zip(*[shifted(4 * i + n) for n in range(4)])
            totals = [t + taps[u, TAPS] for t in sums(0, ms)]
            s1 = [p1] + sums(1, ms)
            totals = [t + jnp.where(d >= 8, p, 0.0) for t, d, p in zip(totals, ds, s1)]
            s2 = [q2, p2] + sums(2, ms)
            totals = [t + jnp.where(d >= 16, p, 0.0) for t, d, p in zip(totals, ds, s2)]
            s3 = [r3, q3, p3] + sums(3, ms)
            totals = [t + jnp.where(d >= 24, p, 0.0) for t, d, p in zip(totals, ds, s3)]
            base = pl.multiple_of(32 * i - TAIL, 32)
            for n in range(4):
                conv[u, pl.ds(base + 8 * n, 8), :] = totals[n].astype(BF16).astype(F32)
            return s1[4], s2[5], s3[6], s2[4], s3[5], s3[4]

        _, m1 = shifted(1)
        _, m2 = shifted(2)
        _, m3 = shifted(3)
        p1 = sums(1, [m3])[0]
        q2, p2 = sums(2, [m2, m3])
        r3, q3, p3 = sums(3, [m1, m2, m3])
        lax.fori_loop(1, ROWS // 32, step, (p1, p2, p3, q2, q3, r3))

    def normalize():
        def step(i, _):
            rows = pl.ds(pl.multiple_of(128 * i, 128), 128)
            total = conv[0, rows, :]
            for u in range(1, 8):
                total = total + conv[u, rows, :]
            mean = jnp.sum(total, axis=1, keepdims=True) * (1.0 / 1024)
            square = None
            for u in range(8):
                off = conv[u, rows, :] - mean
                square = off * off if square is None else square + off * off
            var = jnp.sum(square, axis=1, keepdims=True) * (1.0 / 1024)
            scale = lax.rsqrt(var + 1e-05)
            for u in range(8):
                v = (conv[u, rows, :] - mean) * scale * vecs[1, pl.ds(u, 1), :] + vecs[2, pl.ds(u, 1), :]
                half = 0.5 * v
                act[rows, pl.ds(128 * u, 128)] = (half + half * jnp.tanh(half)).astype(BF16)
            return 0

        lax.fori_loop(0, TOK // 128, step, 0)

    def slot(t, _):
        s = t - LEAD_SEND

        def stage(lead):
            m = s + lead
            return m, jnp.logical_and(m >= 0, m < UNITS)

        m0, on0 = stage(LEAD_SEND)

        @pl.when(on0)
        def _():
            wait(w.at[m0, 0, pc], load_sem.at[m0])
            own = w.at[m0, 0, pc, class_of(kind_of(m0))]
            q = class_of(kind_of(m0))
            for e, dy in ((2, 1), (1, -1), (4, 2), (3, -2)):
                send(own, 0, m0, at(dy=dy), w.at[m0, e, pc, q])
            send(w.at[m0, 0, pc], 4, m0, partner)

        @pl.when(s == -LEAD_FORWARD)
        def _():
            spread_taps()

        m1, on1 = stage(LEAD_FORWARD)

        @pl.when(on1)
        def _():
            q = class_of(kind_of(m1))
            wait(w.at[m1, pl.ds(1, 4), pc, q], recv_sem.at[0, m1])
            send(w.at[m1, 4, pc, q], 1, m1, at(dy=1), w.at[m1, 6, pc, q])
            send(w.at[m1, 3, pc, q], 1, m1, at(dy=-1), w.at[m1, 5, pc, q])
            low, high = pl.ds(0, 16), pl.ds(16, 16)
            send(w.at[m1, 4, pc, q, low, :], 1, m1, at(dy=2), w.at[m1, 7, pc, q, low, :])
            send(w.at[m1, 3, pc, q, high, :], 1, m1, at(dy=-2), w.at[m1, 7, pc, q, high, :])
            in_plane(m1, 1, 4, 2)

        m2, on2 = stage(LEAD_FAR)

        @pl.when(on2)
        def _():
            wait(w.at[m2, pl.ds(5, 3), pc, class_of(kind_of(m2))], recv_sem.at[1, m2])
            in_plane(m2, 5, 3, 3)

        m3, on3 = stage(LEAD_NEAR_PAIR)

        @pl.when(on3)
        def _():
            wait(w.at[m3, pl.ds(1, 3), pc], recv_sem.at[2, m3])
            send(w.at[m3, pl.ds(1, 4), pc], 4, m3, partner)

        m4, on4 = stage(LEAD_FAR_PAIR)

        @pl.when(on4)
        def _():
            wait(w.at[m4, pl.ds(1, 3), pc, pl.ds(0, 3)], recv_sem.at[3, m4])
            send(w.at[m4, pl.ds(5, 3), pc], 5, m4, partner)

        @pl.when(s == 1 - LEAD_FORWARD)
        def _():
            masks()

        @pl.when(s == 0)
        def _():
            wait(x.at[pl.ds(TAIL, TOK), :], misc_sem.at[0])
            wait(x.at[pl.ds(0, TAIL), :], misc_sem.at[7])

        @pl.when(jnp.logical_and(s >= 0, s < IN_UNITS))
        def _():
            wait(w.at[s, pl.ds(0, 5), 1 - pc], recv_sem.at[4, s])
            wait(w.at[s, pl.ds(5, 3), 1 - pc], recv_sem.at[5, s])
            compute(s)

        @pl.when(s == IN_UNITS - 1)
        def _():
            normalize()

        return 0

    lax.fori_loop(0, UNITS - LEAD_FAR_PAIR + LEAD_SEND, slot, 0)

    def rhs_of(e):
        blocks = []
        for v in range(4):
            for h in range(2):
                lanes = pl.ds(128 * h, 128)
                blocks.append(jnp.concatenate(
                    [w[IN_UNITS + v, e, c, :, :, lanes].reshape(128, 128) for c in range(2)], axis=1))
        return jnp.concatenate(blocks, axis=0)

    def project(i, _):
        pair = (2 * i, 2 * i + 1)
        rhs = jnp.concatenate([rhs_of(e) for e in pair], axis=1)
        both = jnp.dot(act[...], rhs, preferred_element_type=F32).astype(BF16)
        for n, e in enumerate(pair):
            dst = pl.multiple_of(256 * ((py + offset_of(e) + NY) % NY), 256)
            out[:, pl.ds(dst, 256)] = both[:, 256 * n : 256 * (n + 1)]
        return 0

    for v in range(IN_UNITS, UNITS):
        wait(w.at[v, pl.ds(0, 5), 1 - pc], recv_sem.at[4, v])
    lax.fori_loop(0, 2, project, 0)
    for v in range(IN_UNITS, UNITS):
        wait(w.at[v, pl.ds(5, 3), 1 - pc], recv_sem.at[5, v])
    lax.fori_loop(2, 4, project, 0)

    wait(w.at[:, pl.ds(1, 4), 0, 0], send_sem.at[0])
    wait(w.at[:, pl.ds(5, 3), 0, 0], send_sem.at[1])
    wait(w.at[:, pl.ds(1, 3), 0], send_sem.at[2])
    wait(w.at[:, pl.ds(1, 3), 0, pl.ds(0, 3)], send_sem.at[3])
    wait(w.at[:, pl.ds(0, 5), 0], send_sem.at[4])
    wait(w.at[:, pl.ds(5, 3), 0], send_sem.at[5])
    wait(x.at[pl.ds(0, TAIL), :], misc_sem.at[6])
    wait(ids.at[:, pl.ds(0, 128)], misc_sem.at[8])


def body(tokens, segments, w_lin, w_gate, w_out, conv_kernel, conv_bias, norm_gain, norm_bias):
    result = pl.pallas_call(
        kernel,
        out_shape=jax.ShapeDtypeStruct((TOK, 2048), BF16),
        in_specs=[pl.BlockSpec(memory_space=pltpu.HBM)] * 9,
        out_specs=pl.BlockSpec(memory_space=pltpu.VMEM),
        scratch_shapes=[
            pltpu.VMEM((UNITS, 8, 2, 4, 32, 256), BF16),
            pltpu.VMEM((ROWS, 2048), BF16),
            pltpu.VMEM((1, 128 + TOK), jnp.int32),
            pltpu.VMEM((128 + TOK, 128), jnp.int32),
            pltpu.VMEM((ROWS, 128), jnp.int32),
            pltpu.VMEM((8, 32, 8, 128), F32),
            pltpu.VMEM((TAPS, 1024), F32),
            pltpu.VMEM((3, 8, 128), F32),
            pltpu.VMEM((8 + ROWS, 128), F32),
            pltpu.VMEM((8, TOK, 128), F32),
            pltpu.VMEM((TOK, 1024), BF16),
            pltpu.SemaphoreType.DMA((UNITS,)),
            pltpu.SemaphoreType.DMA((10,)),
            pltpu.SemaphoreType.DMA((6, UNITS)),
            pltpu.SemaphoreType.DMA((6,)),
        ],
        compiler_params=pltpu.CompilerParams(
            collective_id=0, has_side_effects=True, vmem_limit_bytes=40 * 1024 * 1024
        ),
    )(
        *[pltpu.with_memory_space_constraint(a, pltpu.HBM) for a in (
        tokens[0],
        segments,
        w_lin.reshape(4, 32, 1024),
        w_gate.reshape(4, 32, 1024),
        w_out.reshape(8, 4, 32, 128),
        conv_kernel,
        conv_bias.reshape(8, 128),
        norm_gain.reshape(8, 128),
        norm_bias.reshape(8, 128),
        )]
    )
    return result[None]


def solution(mesh):
    placed = (
        P("dp", "sp", None),
        P("dp", "sp"),
        P("dp", None),
        P("dp", None),
        P(None, "dp"),
        P(),
        P(),
        P(),
        P(),
    )
    return jax.shard_map(
        body, mesh=mesh, in_specs=placed, out_specs=P("dp", "sp", None), check_vma=False
    )
```

```python
import functools

import jax
import jax.numpy as jnp
from jax import lax
from jax.experimental import pallas as pl
from jax.experimental.pallas import tpu as pltpu
from jax.sharding import PartitionSpec as P

MESH = pl.DeviceIdType.MESH
F32, BF16 = jnp.float32, jnp.bfloat16
NX, NY, NZ = 4, 8, 8
UNITS, IN_UNITS = 12, 8
TOK, TAIL, ROWS = 512, 32, 544
TAPS = 31
LEAD_SEND, LEAD_FORWARD, LEAD_FAR, LEAD_NEAR_PAIR, LEAD_FAR_PAIR = 12, 8, 5, 5, 2


def offset_of(e):
    return ((e + 1) // 2) * (2 * (e % 2) - 1)


def kernel(
    tok, seg, wl, wg, wo, ck, cb, ng, nb, out,
    w, x, ids, idc, dist, taps, ckv, vecs, g, conv, act,
    load_sem, misc_sem, recv_sem, send_sem,
):
    sp, dp = lax.axis_index("sp"), lax.axis_index("dp")
    px, pz = sp % NX, sp // NX
    py, pc = dp // 2, dp % 2

    def at(dx=0, dy=0, dz=0):
        return (
            ((pz + dz + NZ) % NZ) * NX + (px + dx + NX) % NX,
            ((py + dy + NY) % NY) * 2 + pc,
        )

    after = ((sp + 1) % (NX * NZ), dp)
    before = ((sp + NX * NZ - 1) % (NX * NZ), dp)
    partner = (sp, py * 2 + 1 - pc)

    def local(src, dst, sem):
        pltpu.make_async_copy(src, dst, sem).start()

    def wait(region, sem):
        pltpu.make_async_copy(region, region, sem).wait()

    for u in range(IN_UNITS):
        lanes = pl.ds(128 * u, 128)
        local(wl.at[:, :, lanes], w.at[u, 0, pc, :, :, pl.ds(0, 128)], load_sem.at[u])
        local(wg.at[:, :, lanes], w.at[u, 0, pc, :, :, pl.ds(128, 128)], load_sem.at[u])
    for e in range(8):
        src = pl.multiple_of(256 * ((py + offset_of(e) + NY) % NY), 256)
        local(tok.at[:, pl.ds(src, 256)], x.at[pl.ds(TAIL, TOK), pl.ds(256 * e, 256)], misc_sem.at[0])
    local(seg, ids.at[:, pl.ds(128, TOK)], misc_sem.at[1])
    for u in range(8):
        local(wo.at[u], w.at[8 + u // 2, 0, pc, :, :, pl.ds(128 * (u % 2), 128)], load_sem.at[8 + u // 2])
    local(ck, ckv, misc_sem.at[2])
    local(cb, vecs.at[0], misc_sem.at[3])
    local(ng, vecs.at[1], misc_sem.at[4])
    local(nb, vecs.at[2], misc_sem.at[5])

    barrier = pltpu.get_barrier_semaphore()
    peers = [at(dy=1), at(dy=-1), at(dy=2), at(dy=-2), at(dx=1), at(dx=-1), at(dz=1), at(dz=-1),
             partner, after, before]
    for peer in peers:
        pl.semaphore_signal(barrier, inc=1, device_id=peer, device_id_type=MESH)
    pl.semaphore_wait(barrier, len(peers))

    def send(ref, kind, unit, peer, dst=None):
        pltpu.make_async_remote_copy(
            src_ref=ref, dst_ref=ref if dst is None else dst,
            send_sem=send_sem.at[kind], recv_sem=recv_sem.at[kind, unit],
            device_id=peer, device_id_type=MESH,
        ).start()

    def kind_of(m):
        return 1 - (((m + 1) * 5) // UNITS - (m * 5) // UNITS)

    for e in range(8):
        src = pl.multiple_of(256 * ((py + offset_of(e) + NY) % NY), 256)
        pltpu.make_async_remote_copy(
            src_ref=tok.at[pl.ds(TOK - TAIL, TAIL), pl.ds(src, 256)],
            dst_ref=x.at[pl.ds(0, TAIL), pl.ds(256 * e, 256)],
            send_sem=misc_sem.at[6], recv_sem=misc_sem.at[7],
            device_id=after, device_id_type=MESH,
        ).start()
    pltpu.make_async_remote_copy(
        src_ref=seg.at[:, pl.ds(TOK - 128, 128)], dst_ref=ids.at[:, pl.ds(0, 128)],
        send_sem=misc_sem.at[8], recv_sem=misc_sem.at[9],
        device_id=after, device_id_type=MESH,
    ).start()

    def class_of(parity):
        return (px * (1 + parity) + pz * (2 - parity)) % 4

    def planes(parity):
        def mix(a, b):
            return tuple((1 - parity) * i + parity * j for i, j in zip(a, b))
        return (mix(at(dx=1), at(dz=1)), mix(at(dx=-1), at(dz=-1)),
                mix(at(dz=1), at(dx=1)), mix(at(dz=-1), at(dx=-1)))

    def in_plane(m, first, count, kind):
        parity = kind_of(m)
        q = class_of(parity)
        heavy_up, heavy_down, light_up, light_down = planes(parity)
        span = pl.ds(first, count)
        whole = w.at[m, span, pc, q]
        send(whole, kind, m, heavy_up)
        send(whole, kind, m, heavy_down)
        send(w.at[m, span, pc, q, pl.ds(0, 16), :], kind, m, light_up)
        send(w.at[m, span, pc, q, pl.ds(16, 16), :], kind, m, light_down)

    def spread_taps():
        wait(ck, misc_sem.at[2])
        wait(cb, misc_sem.at[3])
        wait(ng, misc_sem.at[4])
        wait(nb, misc_sem.at[5])

        def spread(u, _):
            lanes = pl.ds(pl.multiple_of(128 * u, 128), 128)
            for k in range(TAPS):
                taps[u, k] = jnp.broadcast_to(ckv[pl.ds(TAPS - 1 - k, 1), lanes], (8, 128))
            taps[u, TAPS] = jnp.broadcast_to(vecs[0, pl.ds(u, 1), :], (8, 128))
            return 0

        lax.fori_loop(0, 8, spread, 0)
        g[pl.ds(0, 8), :] = jnp.zeros((8, 128), F32)

    def masks():
        wait(seg, misc_sem.at[1])
        wait(ids.at[:, pl.ds(0, 128)], misc_sem.at[9])
        for b in range(5):
            row = ids[:, pl.ds(128 * b, 128)]
            if b == 0:
                row = jnp.where(sp == 0, -1, row)
            idc[pl.ds(128 * b, 128), :] = jnp.broadcast_to(row, (128, 128)).T

        def count(i, _):
            base = pl.multiple_of(8 * i, 8)
            here = idc[pl.ds(base + 96, 8), :]
            total = jnp.zeros((8, 128), jnp.int32)
            for k, more in ((1, 1), (2, 1), (3, 1), (4, 1), (5, 1), (6, 1), (7, 1), (8, 1), (16, 8), (24, 8)):
                total = total + jnp.where(idc[pl.ds(base + 96 - k, 8), :] == here, more, 0)
            dist[pl.ds(base, 8), :] = total
            return 0

        lax.fori_loop(0, ROWS // 8, count, 0)

    def compute(u):
        wu = w[u].reshape(2048, 256)
        half = ROWS // 2
        for i in range(2):
            r = jnp.dot(x[pl.ds(half * i, half), :], wu, preferred_element_type=F32)
            lin = 0.5 * r[:, :128]
            glu = lin + lin * jnp.tanh(0.5 * r[:, 128:])
            g[pl.ds(8 + half * i, half), :] = glu.astype(BF16).astype(F32)

        def shifted(i):
            base = pl.multiple_of(8 * i, 8)
            d = dist[pl.ds(base, 8), :]
            m = [g[pl.ds(base + 8, 8), :]]
            for j in range(1, 8):
                m.append(jnp.where(d >= j, g[pl.ds(base + 8 - j, 8), :], 0.0))
            return d, m

        def sums(j, ms):
            totals = [None] * len(ms)
            for i8 in range(8):
                if 8 * j + i8 < TAPS:
                    tap = taps[u, 8 * j + i8]
                    for n, m in enumerate(ms):
                        term = tap * m[i8]
                        totals[n] = term if totals[n] is None else totals[n] + term
            return totals

        def step(i, carry):
            p1, p2, p3, q2, q3, r3 = carry
            ds, ms = zip(*[shifted(4 * i + n) for n in range(4)])
            totals = [t + taps[u, TAPS] for t in sums(0, ms)]
            s1 = [p1] + sums(1, ms)
            totals = [t + jnp.where(d >= 8, p, 0.0) for t, d, p in zip(totals, ds, s1)]
            s2 = [q2, p2] + sums(2, ms)
            totals = [t + jnp.where(d >= 16, p, 0.0) for t, d, p in zip(totals, ds, s2)]
            s3 = [r3, q3, p3] + sums(3, ms)
            totals = [t + jnp.where(d >= 24, p, 0.0) for t, d, p in zip(totals, ds, s3)]
            base = pl.multiple_of(32 * i - TAIL, 32)
            for n in range(4):
                conv[u, pl.ds(base + 8 * n, 8), :] = totals[n].astype(BF16).astype(F32)
            return s1[4], s2[5], s3[6], s2[4], s3[5], s3[4]

        _, m1 = shifted(1)
        _, m2 = shifted(2)
        _, m3 = shifted(3)
        p1 = sums(1, [m3])[0]
        q2, p2 = sums(2, [m2, m3])
        r3, q3, p3 = sums(3, [m1, m2, m3])
        lax.fori_loop(1, ROWS // 32, step, (p1, p2, p3, q2, q3, r3))

    def normalize():
        def step(i, _):
            rows = pl.ds(pl.multiple_of(128 * i, 128), 128)
            total = conv[0, rows, :]
            for u in range(1, 8):
                total = total + conv[u, rows, :]
            mean = jnp.sum(total, axis=1, keepdims=True) * (1.0 / 1024)
            square = None
            for u in range(8):
                off = conv[u, rows, :] - mean
                square = off * off if square is None else square + off * off
            var = jnp.sum(square, axis=1, keepdims=True) * (1.0 / 1024)
            scale = lax.rsqrt(var + 1e-05)
            for u in range(8):
                v = (conv[u, rows, :] - mean) * scale * vecs[1, pl.ds(u, 1), :] + vecs[2, pl.ds(u, 1), :]
                half = 0.5 * v
                act[rows, pl.ds(128 * u, 128)] = (half + half * jnp.tanh(half)).astype(BF16)
            return 0

        lax.fori_loop(0, TOK // 128, step, 0)

    def slot(t, _):
        s = t - LEAD_SEND

        def stage(lead):
            m = s + lead
            return m, jnp.logical_and(m >= 0, m < UNITS)

        m0, on0 = stage(LEAD_SEND)

        @pl.when(on0)
        def _():
            wait(w.at[m0, 0, pc], load_sem.at[m0])
            own = w.at[m0, 0, pc, class_of(kind_of(m0))]
            q = class_of(kind_of(m0))
            for e, dy in ((2, 1), (1, -1), (4, 2), (3, -2)):
                send(own, 0, m0, at(dy=dy), w.at[m0, e, pc, q])
            send(w.at[m0, 0, pc], 4, m0, partner)

        @pl.when(s == -LEAD_FORWARD)
        def _():
            spread_taps()

        m1, on1 = stage(LEAD_FORWARD)

        @pl.when(on1)
        def _():
            q = class_of(kind_of(m1))
            wait(w.at[m1, pl.ds(1, 4), pc, q], recv_sem.at[0, m1])
            send(w.at[m1, 4, pc, q], 1, m1, at(dy=1), w.at[m1, 6, pc, q])
            send(w.at[m1, 3, pc, q], 1, m1, at(dy=-1), w.at[m1, 5, pc, q])
            low, high = pl.ds(0, 16), pl.ds(16, 16)
            send(w.at[m1, 4, pc, q, low, :], 1, m1, at(dy=2), w.at[m1, 7, pc, q, low, :])
            send(w.at[m1, 3, pc, q, high, :], 1, m1, at(dy=-2), w.at[m1, 7, pc, q, high, :])
            in_plane(m1, 1, 4, 2)

        m2, on2 = stage(LEAD_FAR)

        @pl.when(on2)
        def _():
            wait(w.at[m2, pl.ds(5, 3), pc, class_of(kind_of(m2))], recv_sem.at[1, m2])
            in_plane(m2, 5, 3, 3)

        m3, on3 = stage(LEAD_NEAR_PAIR)

        @pl.when(on3)
        def _():
            wait(w.at[m3, pl.ds(1, 3), pc], recv_sem.at[2, m3])
            send(w.at[m3, pl.ds(1, 4), pc], 4, m3, partner)

        m4, on4 = stage(LEAD_FAR_PAIR)

        @pl.when(on4)
        def _():
            wait(w.at[m4, pl.ds(1, 3), pc, pl.ds(0, 3)], recv_sem.at[3, m4])
            send(w.at[m4, pl.ds(5, 3), pc], 5, m4, partner)

        @pl.when(s == 1 - LEAD_FORWARD)
        def _():
            masks()

        @pl.when(s == 0)
        def _():
            wait(x.at[pl.ds(TAIL, TOK), :], misc_sem.at[0])
            wait(x.at[pl.ds(0, TAIL), :], misc_sem.at[7])

        @pl.when(jnp.logical_and(s >= 0, s < IN_UNITS))
        def _():
            wait(w.at[s, pl.ds(0, 5), 1 - pc], recv_sem.at[4, s])
            wait(w.at[s, pl.ds(5, 3), 1 - pc], recv_sem.at[5, s])
            compute(s)

        return 0

    lax.fori_loop(0, UNITS - LEAD_FAR_PAIR + LEAD_SEND, slot, 0)

    def rhs_of(e):
        blocks = []
        for v in range(4):
            for h in range(2):
                lanes = pl.ds(128 * h, 128)
                blocks.append(jnp.concatenate(
                    [w[IN_UNITS + v, e, c, :, :, lanes].reshape(128, 128) for c in range(2)], axis=1))
        return jnp.concatenate(blocks, axis=0)

    def project(i, _):
        pair = (2 * i, 2 * i + 1)
        rhs = jnp.concatenate([rhs_of(e) for e in pair], axis=1)
        both = jnp.dot(act[...], rhs, preferred_element_type=F32).astype(BF16)
        for n, e in enumerate(pair):
            dst = pl.multiple_of(256 * ((py + offset_of(e) + NY) % NY), 256)
            out[:, pl.ds(dst, 256)] = both[:, 256 * n : 256 * (n + 1)]
        return 0

    normalize()
    for v in range(IN_UNITS, UNITS):
        wait(w.at[v, pl.ds(0, 5), 1 - pc], recv_sem.at[4, v])
    lax.fori_loop(0, 2, project, 0)
    for v in range(IN_UNITS, UNITS):
        wait(w.at[v, pl.ds(5, 3), 1 - pc], recv_sem.at[5, v])
    lax.fori_loop(2, 4, project, 0)

    wait(w.at[:, pl.ds(1, 4), 0, 0], send_sem.at[0])
    wait(w.at[:, pl.ds(5, 3), 0, 0], send_sem.at[1])
    wait(w.at[:, pl.ds(1, 3), 0], send_sem.at[2])
    wait(w.at[:, pl.ds(1, 3), 0, pl.ds(0, 3)], send_sem.at[3])
    wait(w.at[:, pl.ds(0, 5), 0], send_sem.at[4])
    wait(w.at[:, pl.ds(5, 3), 0], send_sem.at[5])
    wait(x.at[pl.ds(0, TAIL), :], misc_sem.at[6])
    wait(ids.at[:, pl.ds(0, 128)], misc_sem.at[8])


def body(tokens, segments, w_lin, w_gate, w_out, conv_kernel, conv_bias, norm_gain, norm_bias):
    result = pl.pallas_call(
        kernel,
        out_shape=jax.ShapeDtypeStruct((TOK, 2048), BF16),
        in_specs=[pl.BlockSpec(memory_space=pltpu.HBM)] * 9,
        out_specs=pl.BlockSpec(memory_space=pltpu.VMEM),
        scratch_shapes=[
            pltpu.VMEM((UNITS, 8, 2, 4, 32, 256), BF16),
            pltpu.VMEM((ROWS, 2048), BF16),
            pltpu.VMEM((1, 128 + TOK), jnp.int32),
            pltpu.VMEM((128 + TOK, 128), jnp.int32),
            pltpu.VMEM((ROWS, 128), jnp.int32),
            pltpu.VMEM((8, 32, 8, 128), F32),
            pltpu.VMEM((TAPS, 1024), F32),
            pltpu.VMEM((3, 8, 128), F32),
            pltpu.VMEM((8 + ROWS, 128), F32),
            pltpu.VMEM((8, TOK, 128), F32),
            pltpu.VMEM((TOK, 1024), BF16),
            pltpu.SemaphoreType.DMA((UNITS,)),
            pltpu.SemaphoreType.DMA((10,)),
            pltpu.SemaphoreType.DMA((6, UNITS)),
            pltpu.SemaphoreType.DMA((6,)),
        ],
        compiler_params=pltpu.CompilerParams(
            collective_id=0, has_side_effects=True, vmem_limit_bytes=40 * 1024 * 1024
        ),
    )(
        *[pltpu.with_memory_space_constraint(a, pltpu.HBM) for a in (
        tokens[0],
        segments,
        w_lin.reshape(4, 32, 1024),
        w_gate.reshape(4, 32, 1024),
        w_out.reshape(8, 4, 32, 128),
        conv_kernel,
        conv_bias.reshape(8, 128),
        norm_gain.reshape(8, 128),
        norm_bias.reshape(8, 128),
        )]
    )
    return result[None]


def solution(mesh):
    placed = (
        P("dp", "sp", None),
        P("dp", "sp"),
        P("dp", None),
        P("dp", None),
        P(None, "dp"),
        P(),
        P(),
        P(),
        P(),
    )
    return jax.shard_map(
        body, mesh=mesh, in_specs=placed, out_specs=P("dp", "sp", None), check_vma=False
    )
```

```python
import functools

import jax
import jax.numpy as jnp
from jax import lax
from jax.experimental import pallas as pl
from jax.experimental.pallas import tpu as pltpu
from jax.sharding import PartitionSpec as P

MESH = pl.DeviceIdType.MESH
F32, BF16 = jnp.float32, jnp.bfloat16
NX, NY, NZ = 4, 8, 8
UNITS, IN_UNITS = 12, 8
TOK, TAIL, ROWS = 512, 32, 544
TAPS = 31
LEAD_SEND, LEAD_FORWARD, LEAD_FAR, LEAD_NEAR_PAIR, LEAD_FAR_PAIR = 12, 8, 5, 5, 2


def offset_of(e):
    return ((e + 1) // 2) * (2 * (e % 2) - 1)


def kernel(
    tok, seg, wl, wg, wo, ck, cb, ng, nb, out,
    w, x, ids, idc, dist, taps, ckv, vecs, g, conv, act,
    load_sem, misc_sem, recv_sem, send_sem,
):
    sp, dp = lax.axis_index("sp"), lax.axis_index("dp")
    px, pz = sp % NX, sp // NX
    py, pc = dp // 2, dp % 2

    def at(dx=0, dy=0, dz=0):
        return (
            ((pz + dz + NZ) % NZ) * NX + (px + dx + NX) % NX,
            ((py + dy + NY) % NY) * 2 + pc,
        )

    after = ((sp + 1) % (NX * NZ), dp)
    before = ((sp + NX * NZ - 1) % (NX * NZ), dp)
    partner = (sp, py * 2 + 1 - pc)

    def local(src, dst, sem):
        pltpu.make_async_copy(src, dst, sem).start()

    def wait(region, sem):
        pltpu.make_async_copy(region, region, sem).wait()

    for u in range(IN_UNITS):
        lanes = pl.ds(128 * u, 128)
        local(wl.at[:, :, lanes], w.at[u, 0, pc, :, :, pl.ds(0, 128)], load_sem.at[u])
        local(wg.at[:, :, lanes], w.at[u, 0, pc, :, :, pl.ds(128, 128)], load_sem.at[u])
    for e in range(8):
        src = pl.multiple_of(256 * ((py + offset_of(e) + NY) % NY), 256)
        local(tok.at[:, pl.ds(src, 256)], x.at[pl.ds(TAIL, TOK), pl.ds(256 * e, 256)], misc_sem.at[0])
    local(seg, ids.at[:, pl.ds(128, TOK)], misc_sem.at[1])
    for u in range(8):
        local(wo.at[u], w.at[8 + u // 2, 0, pc, :, :, pl.ds(128 * (u % 2), 128)], load_sem.at[8 + u // 2])
    local(ck, ckv, misc_sem.at[2])
    local(cb, vecs.at[0], misc_sem.at[3])
    local(ng, vecs.at[1], misc_sem.at[4])
    local(nb, vecs.at[2], misc_sem.at[5])

    barrier = pltpu.get_barrier_semaphore()
    peers = [at(dy=1), at(dy=-1), at(dy=2), at(dy=-2), at(dx=1), at(dx=-1), at(dz=1), at(dz=-1),
             partner, after, before]
    for peer in peers:
        pl.semaphore_signal(barrier, inc=1, device_id=peer, device_id_type=MESH)
    pl.semaphore_wait(barrier, len(peers))

    def send(ref, kind, unit, peer, dst=None):
        pltpu.make_async_remote_copy(
            src_ref=ref, dst_ref=ref if dst is None else dst,
            send_sem=send_sem.at[kind], recv_sem=recv_sem.at[kind, unit],
            device_id=peer, device_id_type=MESH,
        ).start()

    def kind_of(m):
        return 1 - (((m + 1) * 5) // UNITS - (m * 5) // UNITS)

    for e in range(8):
        src = pl.multiple_of(256 * ((py + offset_of(e) + NY) % NY), 256)
        pltpu.make_async_remote_copy(
            src_ref=tok.at[pl.ds(TOK - TAIL, TAIL), pl.ds(src, 256)],
            dst_ref=x.at[pl.ds(0, TAIL), pl.ds(256 * e, 256)],
            send_sem=misc_sem.at[6], recv_sem=misc_sem.at[7],
            device_id=after, device_id_type=MESH,
        ).start()
    pltpu.make_async_remote_copy(
        src_ref=seg.at[:, pl.ds(TOK - 128, 128)], dst_ref=ids.at[:, pl.ds(0, 128)],
        send_sem=misc_sem.at[8], recv_sem=misc_sem.at[9],
        device_id=after, device_id_type=MESH,
    ).start()

    def class_of(parity):
        return (px * (1 + parity) + pz * (2 - parity)) % 4

    def planes(parity):
        def mix(a, b):
            return tuple((1 - parity) * i + parity * j for i, j in zip(a, b))
        return (mix(at(dx=1), at(dz=1)), mix(at(dx=-1), at(dz=-1)),
                mix(at(dz=1), at(dx=1)), mix(at(dz=-1), at(dx=-1)))

    def in_plane(m, first, count, kind):
        parity = kind_of(m)
        q = class_of(parity)
        heavy_up, heavy_down, light_up, light_down = planes(parity)
        span = pl.ds(first, count)
        whole = w.at[m, span, pc, q]
        send(whole, kind, m, heavy_up)
        send(whole, kind, m, heavy_down)
        send(w.at[m, span, pc, q, pl.ds(0, 16), :], kind, m, light_up)
        send(w.at[m, span, pc, q, pl.ds(16, 16), :], kind, m, light_down)

    def spread_taps():
        wait(ck, misc_sem.at[2])
        wait(cb, misc_sem.at[3])
        wait(ng, misc_sem.at[4])
        wait(nb, misc_sem.at[5])

        def spread(u, _):
            lanes = pl.ds(pl.multiple_of(128 * u, 128), 128)
            for k in range(TAPS):
                taps[u, k] = jnp.broadcast_to(ckv[pl.ds(TAPS - 1 - k, 1), lanes], (8, 128))
            taps[u, TAPS] = jnp.broadcast_to(vecs[0, pl.ds(u, 1), :], (8, 128))
            return 0

        lax.fori_loop(0, 8, spread, 0)
        g[pl.ds(0, 8), :] = jnp.zeros((8, 128), F32)

    def masks():
        wait(seg, misc_sem.at[1])
        wait(ids.at[:, pl.ds(0, 128)], misc_sem.at[9])
        for b in range(5):
            row = ids[:, pl.ds(128 * b, 128)]
            if b == 0:
                row = jnp.where(sp == 0, -1, row)
            idc[pl.ds(128 * b, 128), :] = jnp.broadcast_to(row, (128, 128)).T

        def count(i, _):
            base = pl.multiple_of(8 * i, 8)
            here = idc[pl.ds(base + 96, 8), :]
            total = jnp.zeros((8, 128), jnp.int32)
            for k, more in ((1, 1), (2, 1), (3, 1), (4, 1), (5, 1), (6, 1), (7, 1), (8, 1), (16, 8), (24, 8)):
                total = total + jnp.where(idc[pl.ds(base + 96 - k, 8), :] == here, more, 0)
            dist[pl.ds(base, 8), :] = total
            return 0

        lax.fori_loop(0, ROWS // 8, count, 0)

    def gate_unit(u):
        wu = w[u].reshape(2048, 256)
        half = ROWS // 2
        for i in range(2):
            r = jnp.dot(x[pl.ds(half * i, half), :], wu, preferred_element_type=F32)
            lin = 0.5 * r[:, :128]
            glu = lin + lin * jnp.tanh(0.5 * r[:, 128:])
            g[pl.ds(8 + half * i, half), :] = glu.astype(BF16).astype(F32)

    def convolve(u):
        def shifted(i):
            base = pl.multiple_of(8 * i, 8)
            d = dist[pl.ds(base, 8), :]
            m = [g[pl.ds(base + 8, 8), :]]
            for j in range(1, 8):
                m.append(jnp.where(d >= j, g[pl.ds(base + 8 - j, 8), :], 0.0))
            return d, m

        def sums(j, ms):
            totals = [None] * len(ms)
            for i8 in range(8):
                if 8 * j + i8 < TAPS:
                    tap = taps[u, 8 * j + i8]
                    for n, m in enumerate(ms):
                        term = tap * m[i8]
                        totals[n] = term if totals[n] is None else totals[n] + term
            return totals

        def step(i, carry):
            p1, p2, p3, q2, q3, r3 = carry
            ds, ms = zip(*[shifted(4 * i + n) for n in range(4)])
            totals = [t + taps[u, TAPS] for t in sums(0, ms)]
            s1 = [p1] + sums(1, ms)
            totals = [t + jnp.where(d >= 8, p, 0.0) for t, d, p in zip(totals, ds, s1)]
            s2 = [q2, p2] + sums(2, ms)
            totals = [t + jnp.where(d >= 16, p, 0.0) for t, d, p in zip(totals, ds, s2)]
            s3 = [r3, q3, p3] + sums(3, ms)
            totals = [t + jnp.where(d >= 24, p, 0.0) for t, d, p in zip(totals, ds, s3)]
            base = pl.multiple_of(32 * i - TAIL, 32)
            for n in range(4):
                conv[u, pl.ds(base + 8 * n, 8), :] = totals[n].astype(BF16).astype(F32)
            return s1[4], s2[5], s3[6], s2[4], s3[5], s3[4]

        _, m1 = shifted(1)
        _, m2 = shifted(2)
        _, m3 = shifted(3)
        p1 = sums(1, [m3])[0]
        q2, p2 = sums(2, [m2, m3])
        r3, q3, p3 = sums(3, [m1, m2, m3])
        lax.fori_loop(1, ROWS // 32, step, (p1, p2, p3, q2, q3, r3))

    def normalize():
        def step(i, _):
            rows = pl.ds(pl.multiple_of(128 * i, 128), 128)
            total = conv[0, rows, :]
            for u in range(1, 8):
                total = total + conv[u, rows, :]
            mean = jnp.sum(total, axis=1, keepdims=True) * (1.0 / 1024)
            square = None
            for u in range(8):
                off = conv[u, rows, :] - mean
                square = off * off if square is None else square + off * off
            var = jnp.sum(square, axis=1, keepdims=True) * (1.0 / 1024)
            scale = lax.rsqrt(var + 1e-05)
            for u in range(8):
                v = (conv[u, rows, :] - mean) * scale * vecs[1, pl.ds(u, 1), :] + vecs[2, pl.ds(u, 1), :]
                half = 0.5 * v
                act[rows, pl.ds(128 * u, 128)] = (half + half * jnp.tanh(half)).astype(BF16)
            return 0

        lax.fori_loop(0, TOK // 128, step, 0)

    def slot(t, _):
        s = t - LEAD_SEND

        def stage(lead):
            m = s + lead
            return m, jnp.logical_and(m >= 0, m < UNITS)

        m0, on0 = stage(LEAD_SEND)

        @pl.when(on0)
        def _():
            wait(w.at[m0, 0, pc], load_sem.at[m0])
            own = w.at[m0, 0, pc, class_of(kind_of(m0))]
            q = class_of(kind_of(m0))
            for e, dy in ((2, 1), (1, -1), (4, 2), (3, -2)):
                send(own, 0, m0, at(dy=dy), w.at[m0, e, pc, q])
            send(w.at[m0, 0, pc], 4, m0, partner)

        @pl.when(s == -LEAD_FORWARD)
        def _():
            spread_taps()

        m1, on1 = stage(LEAD_FORWARD)

        @pl.when(on1)
        def _():
            q = class_of(kind_of(m1))
            wait(w.at[m1, pl.ds(1, 4), pc, q], recv_sem.at[0, m1])
            send(w.at[m1, 4, pc, q], 1, m1, at(dy=1), w.at[m1, 6, pc, q])
            send(w.at[m1, 3, pc, q], 1, m1, at(dy=-1), w.at[m1, 5, pc, q])
            low, high = pl.ds(0, 16), pl.ds(16, 16)
            send(w.at[m1, 4, pc, q, low, :], 1, m1, at(dy=2), w.at[m1, 7, pc, q, low, :])
            send(w.at[m1, 3, pc, q, high, :], 1, m1, at(dy=-2), w.at[m1, 7, pc, q, high, :])
            in_plane(m1, 1, 4, 2)

        @pl.when(s == 0)
        def _():
            wait(x.at[pl.ds(TAIL, TOK), :], misc_sem.at[0])
            wait(x.at[pl.ds(0, TAIL), :], misc_sem.at[7])

        @pl.when(jnp.logical_and(s >= 0, s < IN_UNITS))
        def _():
            wait(w.at[s, pl.ds(0, 5), 1 - pc], recv_sem.at[4, s])
            wait(w.at[s, pl.ds(5, 3), 1 - pc], recv_sem.at[5, s])
            gate_unit(s)

        m2, on2 = stage(LEAD_FAR)

        @pl.when(on2)
        def _():
            wait(w.at[m2, pl.ds(5, 3), pc, class_of(kind_of(m2))], recv_sem.at[1, m2])
            in_plane(m2, 5, 3, 3)

        m3, on3 = stage(LEAD_NEAR_PAIR)

        @pl.when(on3)
        def _():
            wait(w.at[m3, pl.ds(1, 3), pc], recv_sem.at[2, m3])
            send(w.at[m3, pl.ds(1, 4), pc], 4, m3, partner)

        m4, on4 = stage(LEAD_FAR_PAIR)

        @pl.when(on4)
        def _():
            wait(w.at[m4, pl.ds(1, 3), pc, pl.ds(0, 3)], recv_sem.at[3, m4])
            send(w.at[m4, pl.ds(5, 3), pc], 5, m4, partner)

        @pl.when(s == 1 - LEAD_FORWARD)
        def _():
            masks()

        @pl.when(jnp.logical_and(s >= 0, s < IN_UNITS))
        def _():
            convolve(s)

        return 0

    lax.fori_loop(0, UNITS - LEAD_FAR_PAIR + LEAD_SEND, slot, 0)

    def rhs_of(e):
        blocks = []
        for v in range(4):
            for h in range(2):
                lanes = pl.ds(128 * h, 128)
                blocks.append(jnp.concatenate(
                    [w[IN_UNITS + v, e, c, :, :, lanes].reshape(128, 128) for c in range(2)], axis=1))
        return jnp.concatenate(blocks, axis=0)

    def project(i, _):
        pair = (2 * i, 2 * i + 1)
        rhs = jnp.concatenate([rhs_of(e) for e in pair], axis=1)
        both = jnp.dot(act[...], rhs, preferred_element_type=F32).astype(BF16)
        for n, e in enumerate(pair):
            dst = pl.multiple_of(256 * ((py + offset_of(e) + NY) % NY), 256)
            out[:, pl.ds(dst, 256)] = both[:, 256 * n : 256 * (n + 1)]
        return 0

    normalize()
    for v in range(IN_UNITS, UNITS):
        wait(w.at[v, pl.ds(0, 5), 1 - pc], recv_sem.at[4, v])
    lax.fori_loop(0, 2, project, 0)
    for v in range(IN_UNITS, UNITS):
        wait(w.at[v, pl.ds(5, 3), 1 - pc], recv_sem.at[5, v])
    lax.fori_loop(2, 4, project, 0)

    wait(w.at[:, pl.ds(1, 4), 0, 0], send_sem.at[0])
    wait(w.at[:, pl.ds(5, 3), 0, 0], send_sem.at[1])
    wait(w.at[:, pl.ds(1, 3), 0], send_sem.at[2])
    wait(w.at[:, pl.ds(1, 3), 0, pl.ds(0, 3)], send_sem.at[3])
    wait(w.at[:, pl.ds(0, 5), 0], send_sem.at[4])
    wait(w.at[:, pl.ds(5, 3), 0], send_sem.at[5])
    wait(x.at[pl.ds(0, TAIL), :], misc_sem.at[6])
    wait(ids.at[:, pl.ds(0, 128)], misc_sem.at[8])


def body(tokens, segments, w_lin, w_gate, w_out, conv_kernel, conv_bias, norm_gain, norm_bias):
    result = pl.pallas_call(
        kernel,
        out_shape=jax.ShapeDtypeStruct((TOK, 2048), BF16),
        in_specs=[pl.BlockSpec(memory_space=pltpu.HBM)] * 9,
        out_specs=pl.BlockSpec(memory_space=pltpu.VMEM),
        scratch_shapes=[
            pltpu.VMEM((UNITS, 8, 2, 4, 32, 256), BF16),
            pltpu.VMEM((ROWS, 2048), BF16),
            pltpu.VMEM((1, 128 + TOK), jnp.int32),
            pltpu.VMEM((128 + TOK, 128), jnp.int32),
            pltpu.VMEM((ROWS, 128), jnp.int32),
            pltpu.VMEM((8, 32, 8, 128), F32),
            pltpu.VMEM((TAPS, 1024), F32),
            pltpu.VMEM((3, 8, 128), F32),
            pltpu.VMEM((8 + ROWS, 128), F32),
            pltpu.VMEM((8, TOK, 128), F32),
            pltpu.VMEM((TOK, 1024), BF16),
            pltpu.SemaphoreType.DMA((UNITS,)),
            pltpu.SemaphoreType.DMA((10,)),
            pltpu.SemaphoreType.DMA((6, UNITS)),
            pltpu.SemaphoreType.DMA((6,)),
        ],
        compiler_params=pltpu.CompilerParams(
            collective_id=0, has_side_effects=True, vmem_limit_bytes=40 * 1024 * 1024
        ),
    )(
        *[pltpu.with_memory_space_constraint(a, pltpu.HBM) for a in (
        tokens[0],
        segments,
        w_lin.reshape(4, 32, 1024),
        w_gate.reshape(4, 32, 1024),
        w_out.reshape(8, 4, 32, 128),
        conv_kernel,
        conv_bias.reshape(8, 128),
        norm_gain.reshape(8, 128),
        norm_bias.reshape(8, 128),
        )]
    )
    return result[None]


def solution(mesh):
    placed = (
        P("dp", "sp", None),
        P("dp", "sp"),
        P("dp", None),
        P("dp", None),
        P(None, "dp"),
        P(),
        P(),
        P(),
        P(),
    )
    return jax.shard_map(
        body, mesh=mesh, in_specs=placed, out_specs=P("dp", "sp", None), check_vma=False
    )
```
